32 devices in a mesh: sp: 8 (over z, y), tp: 4 (over x, core).
Axes of the slice: x: 2, y: 2, z: 4, core: 2. Of those that a mesh axis runs over, the one named last changes fastest.
Arguments:
- queries_nope: bfloat16 [3072, 8, 128], P('sp', 'tp'), may hold values from -9 to 9
- queries_rope: bfloat16 [3072, 8, 64], P('sp', 'tp'), may hold values from -6 to 6
- latent: bfloat16 [3072, 512], P('sp'), may hold values from -8 to 8, as said below
- rope_key: bfloat16 [3072, 64], P('sp'), may hold values from -6 to 6
- latent_gain: float32 [512], replicated, may hold values from 0.1 to 1.9
- key_up: bfloat16 [512, 1024], P(None, 'tp'), may hold values from -0.25 to 0.25
- value_up: bfloat16 [512, 1024], P(None, 'tp'), may hold values from -0.25 to 0.25
- out_proj: bfloat16 [1024, 2048], P('tp'), may hold values from -0.75 to 0.75
- stream: bfloat16 [3072, 2048], P(('sp', 'tp')), may hold values from -6 to 6
- mix_gain: float32 [2048], replicated, may hold values from 0.1 to 1.9
- w_gate: bfloat16 [2048, 3072], P('sp', 'tp'), may hold values from -0.125 to 0.125
- w_up: bfloat16 [2048, 3072], P('sp', 'tp'), may hold values from -0.125 to 0.125
- w_down: bfloat16 [3072, 2048], P('tp', 'sp'), may hold values from -0.4375 to 0.4375
- mlp_gain: float32 [2048], replicated, may hold values from 0.1 to 1.9
Outputs:
- result: bfloat16 [3072, 2048], P(('sp', 'tp'))
The draws below stay inside these ranges and needn't reach their ends.
Inputs may be any that keep to these rules, and one draw needn't show every extreme that they name: latent rows carry a mean vector that changes from one eighth of the sequence to the next.
All inputs are finite; a program needn't handle non-finite values.
Results may differ from the reference program's by a relative error of at most 0.017.
Values may be sent and summed in bfloat16 or wider, within the bound.
A program may use at most 192 MiB of HBM per device.

```python
import math
import jax
import jax.numpy as jnp
from jax import lax

D = 2048
HEADS = 8
HEAD = 128
ROPE = 64
LATENT = 512
FF = 3072
SEQ = 3072


def draw_latent(key, part):
    base = jax.random.fold_in(key, 11)
    noise_key, centre_key, factor_key = jax.random.split(base, 3)
    places = jnp.arange(SEQ, dtype=jnp.int32)
    segment = places * 8 // SEQ
    centres = jax.random.normal(centre_key, (8, LATENT), jnp.float32) * 1.5
    noise = jax.random.normal(noise_key, (SEQ, LATENT), jnp.float32)
    return jnp.clip(noise + centres[segment], -8.0, 8.0).astype(jnp.bfloat16)


def rope_pair(key):
    base = jax.random.fold_in(key, 23)
    first_key, second_key, third_key = jax.random.split(base, 3)
    key_part = jnp.clip(jax.random.normal(first_key, (SEQ, ROPE), jnp.float32), -6.0, 6.0)
    query_part = jnp.clip(jax.random.normal(second_key, (SEQ, HEADS, ROPE), jnp.float32), -6.0, 6.0)
    return (query_part.astype(jnp.bfloat16), key_part.astype(jnp.bfloat16))


def draw_queries_rope(key, part):
    return rope_pair(key)[0]


def draw_rope_key(key, part):
    return rope_pair(key)[1]


def levels(own_key, dims, cuts, least, high):
    def one(dim, shards_of):
        heights = jax.random.uniform(jax.random.fold_in(jax.random.fold_in(own_key, 6), dim), (shards_of,), jnp.float32, least / len(cuts), high / len(cuts))
        return jnp.repeat(jnp.exp(heights), dims[dim] // shards_of).reshape((-1,) + (1,) * (len(dims) - dim - 1))

    factor_of = one(*cuts[0])
    for cut in cuts[1:]:
        factor_of = factor_of * one(*cut)
    return factor_of


def normal_values(own_key, dims, scale, reach, shards=(), held_as=jnp.bfloat16):
    loudness = levels(own_key, dims, shards, -0.22, 0.18) if shards else 1.0
    drawn = jax.random.normal(own_key, dims, jnp.float32) * scale * loudness
    return jnp.minimum(jnp.maximum(drawn, -reach), reach).astype(held_as)


def setup_inputs(seed: int = 0) -> dict:
    seeds = jax.random.split(jax.random.key(seed), 15)
    queries_nope = normal_values(seeds[0], (SEQ, HEADS, HEAD), 3.0, 9.0, ((0, 8), (1, 4)))
    queries_rope = draw_queries_rope(jax.random.fold_in(seeds[14], 71), 0)
    latent = draw_latent(jax.random.fold_in(seeds[14], 71), 0)
    rope_key = draw_rope_key(jax.random.fold_in(seeds[14], 71), 0)
    latent_gain = jnp.clip(1.0 + 0.18 * jax.random.normal(seeds[4], (LATENT,), jnp.float32), 0.1, 1.9)
    key_up = normal_values(seeds[5], (LATENT, HEADS * HEAD), LATENT ** -0.5, 0.25, ((1, 4),))
    value_up = normal_values(seeds[6], (LATENT, HEADS * HEAD), LATENT ** -0.5, 0.25, ((1, 4),))
    out_proj = normal_values(seeds[7], (HEADS * HEAD, D), (HEADS * HEAD // 16) ** -0.5, 0.75, ((0, 4),))
    stream = normal_values(seeds[8], (SEQ, D), 1.0, 6.0, ((0, 32),))
    mix_gain = jnp.clip(1.0 + 0.18 * jax.random.normal(seeds[9], (D,), jnp.float32), 0.1, 1.9)
    w_gate = normal_values(seeds[10], (D, FF), D ** -0.5, 0.125, ((0, 8), (1, 4)))
    w_up = normal_values(seeds[11], (D, FF), D ** -0.5, 0.125, ((0, 8), (1, 4)))
    w_down = normal_values(seeds[12], (FF, D), (FF // 16) ** -0.5, 0.4375, ((0, 4), (1, 8)))
    mlp_gain = jnp.clip(1.0 + 0.18 * jax.random.normal(seeds[13], (D,), jnp.float32), 0.1, 1.9)
    return dict(queries_nope=queries_nope, queries_rope=queries_rope, latent=latent, rope_key=rope_key, latent_gain=latent_gain, key_up=key_up, value_up=value_up, out_proj=out_proj, stream=stream, mix_gain=mix_gain, w_gate=w_gate, w_up=w_up, w_down=w_down, mlp_gain=mlp_gain)


theta_base = 10000.0
residual_weight = 8.0 ** 0.25
norm_floor = 1.0
big_negative = -1e+30

def rotate(vector, first_row):
    half = vector.shape[-1] // 2
    rates = theta_base ** (-2.0 * jnp.arange(half, dtype=jnp.float32) / vector.shape[-1])
    places = (first_row + jnp.arange(vector.shape[0], dtype=jnp.int32)).astype(jnp.float32)
    angle = places[:, None] * rates[None, :]
    angle = angle.reshape((vector.shape[0],) + (1,) * (vector.ndim - 2) + (half,))
    cosine = jnp.cos(angle)
    sine = jnp.sin(angle)
    left = vector[..., :half]
    right = vector[..., half:]
    return jnp.concatenate([left * cosine - right * sine, left * sine + right * cosine], axis=-1)

def latent_norm(latent, latent_gain):
    wide = latent.astype(jnp.float32)
    factor = lax.rsqrt(lax.optimization_barrier(jnp.mean(wide * wide, axis=-1, keepdims=True)) + norm_floor)
    return (wide * factor * latent_gain).astype(jnp.bfloat16)

def layer_norm(values, gain):
    centre = lax.optimization_barrier(jnp.mean(values, axis=-1, keepdims=True))
    centred = values - centre
    spread = lax.optimization_barrier(jnp.mean(centred * centred, axis=-1, keepdims=True))
    return centred * lax.rsqrt(spread + norm_floor) * gain

def widen(array):
    return lax.optimization_barrier(array).astype(jnp.float32)

def reference(queries_nope, queries_rope, latent, rope_key, latent_gain, key_up, value_up, out_proj, stream, mix_gain, w_gate, w_up, w_down, mlp_gain):
    seq_len, head_count, head_dim = queries_nope.shape
    rope_dim = queries_rope.shape[2]
    query_turned = rotate(queries_rope.astype(jnp.float32), 0).astype(jnp.bfloat16)
    key_turned = rotate(rope_key.astype(jnp.float32), 0).astype(jnp.bfloat16)
    normed = latent_norm(latent, latent_gain)
    keys = jnp.dot(normed, key_up, preferred_element_type=jnp.float32).astype(jnp.bfloat16)
    keys = widen(keys).reshape(seq_len, head_count, head_dim)
    values_all = jnp.dot(normed, value_up, preferred_element_type=jnp.float32).astype(jnp.bfloat16)
    values_all = widen(values_all).reshape(seq_len, head_count, head_dim)
    key_wide = key_turned.astype(jnp.float32)
    scale = (head_dim + rope_dim) ** (-0.5)
    block = math.gcd(seq_len, 512)
    key_places = jnp.arange(seq_len, dtype=jnp.int32)

    def one_block(index):
        begin = (index * block).astype(jnp.int32)
        query_block = lax.dynamic_slice_in_dim(queries_nope, begin, block, 0).astype(jnp.float32)
        turned_block = lax.dynamic_slice_in_dim(query_turned, begin, block, 0).astype(jnp.float32)
        score = jnp.einsum('thd,shd->hts', query_block, keys) + jnp.einsum('thr,sr->hts', turned_block, key_wide)
        score = score * scale
        allowed = key_places[None, :] <= (begin + jnp.arange(block, dtype=jnp.int32))[:, None]
        score = jnp.where(allowed[None], score, big_negative)
        top = lax.optimization_barrier(jnp.max(score, axis=2, keepdims=True))
        powers = jnp.exp(score - top) * allowed[None]
        denominators = lax.optimization_barrier(jnp.sum(powers, axis=2))
        summed = jnp.einsum('hts,shd->thd', widen(powers.astype(jnp.bfloat16)), values_all)
        return (summed / denominators.T[:, :, None]).astype(jnp.bfloat16)
    blocks = lax.map(one_block, jnp.arange(seq_len // block, dtype=jnp.int32))
    attended = blocks.reshape(seq_len, head_count * head_dim)
    projected = jnp.dot(attended, out_proj, preferred_element_type=jnp.float32)
    mixed = layer_norm(residual_weight * stream.astype(jnp.float32) + projected, mix_gain).astype(jnp.bfloat16)
    gate_sum = jnp.dot(mixed, w_gate, preferred_element_type=jnp.float32)
    up_sum = jnp.dot(mixed, w_up, preferred_element_type=jnp.float32)
    hidden = (jax.nn.silu(gate_sum) * up_sum).astype(jnp.bfloat16)
    lowered = jnp.dot(hidden, w_down, preferred_element_type=jnp.float32)
    return layer_norm(residual_weight * mixed.astype(jnp.float32) + 0.5 * lowered, mlp_gain).astype(jnp.bfloat16)
```

```python
import functools

import jax
import jax.numpy as jnp
from jax import lax
from jax.experimental import pallas as pl
from jax.experimental.pallas import tpu as pltpu
from jax.sharding import PartitionSpec as P

theta_base = 10000.0
residual_weight = 8.0**0.25
norm_floor = 1.0
big_negative = -1e30


def rotate(vector, first_row):
    half = vector.shape[-1] // 2
    rates = theta_base ** (-2.0 * jnp.arange(half, dtype=jnp.float32) / vector.shape[-1])
    places = (first_row + jnp.arange(vector.shape[0], dtype=jnp.int32)).astype(jnp.float32)
    angle = places[:, None] * rates[None, :]
    angle = angle.reshape((vector.shape[0],) + (1,) * (vector.ndim - 2) + (half,))
    cosine = jnp.cos(angle)
    sine = jnp.sin(angle)
    left = vector[..., :half]
    right = vector[..., half:]
    return jnp.concatenate([left * cosine - right * sine, left * sine + right * cosine], axis=-1)


def latent_norm(latent, latent_gain):
    wide = latent.astype(jnp.float32)
    factor = lax.rsqrt(jnp.mean(wide * wide, axis=-1, keepdims=True) + norm_floor)
    return (wide * factor * latent_gain).astype(jnp.bfloat16)


def layer_norm(values, gain):
    centre = jnp.mean(values, axis=-1, keepdims=True)
    centred = values - centre
    spread = jnp.mean(centred * centred, axis=-1, keepdims=True)
    return centred * lax.rsqrt(spread + norm_floor) * gain


mesh_id = pl.DeviceIdType.MESH
bf16 = jnp.bfloat16
f32 = jnp.float32


def layer_kernel(
    chain,
    teams,
    scale,
    qcat,
    latent_in,
    key_up,
    value_up,
    proj_in,
    stream,
    mix_gain,
    gate_in,
    up_in,
    down_in,
    mlp_gain,
    result,
    lat,
    gate,
    up,
    down,
    proj,
    heads_out,
    heads_in,
    rows,
    hidden,
    terms,
    arrived,
    wide,
    top,
    total,
    weighted,
    local_sem,
    lat_recv,
    lat_up,
    lat_side,
    lat_core,
    w_recv,
    w_side,
    w_up,
    w_down,
    proj_recv,
    proj_send,
    head_recv,
    head_send,
    row_recv,
    row_send,
    term_recv,
    term_send,
):
    sp = lax.axis_index("sp")
    t = lax.axis_index("tp")
    q = sp // 2
    p = sp % 2
    other = 1 - p
    half = t % 2
    mate = t + 1 - 2 * half
    group = 2 * teams
    mine = p * teams + t
    last = chain - 1
    head_count = qcat.shape[0]
    head_dim = value_up.shape[1] // head_count
    block_rows = qcat.shape[1]
    width = value_up.shape[0]
    has_up = q < last
    has_down = q > 0

    def place(pp, tt, qq=None):
        return ((q if qq is None else qq) * 2 + pp, tt)

    def remote(source, target, send, recv, device):
        return pltpu.make_async_remote_copy(
            src_ref=source,
            dst_ref=target,
            send_sem=send,
            recv_sem=recv,
            device_id=device,
            device_id_type=mesh_id,
        )

    barrier = pltpu.get_barrier_semaphore()
    for step in range(1, group):
        index = lax.rem(mine + step, group)
        pl.semaphore_signal(
            barrier, inc=1, device_id=place(index // teams, index % teams), device_id_type=mesh_id
        )

    @pl.when(has_up)
    def _():
        pl.semaphore_signal(barrier, inc=1, device_id=place(p, t, q + 1), device_id_type=mesh_id)

    @pl.when(has_down)
    def _():
        pl.semaphore_signal(barrier, inc=1, device_id=place(p, t, q - 1), device_id_type=mesh_id)

    peers = group - 1 + jnp.where(has_up, 1, 0) + jnp.where(has_down, 1, 0)
    pl.semaphore_wait(barrier, peers)

    def lat_to_up(j, source):
        return remote(
            source, lat.at[j, p, half], lat_up.at[j], lat_recv.at[j, p, half], place(p, t, q + 1)
        )

    def lat_to_side(j, source):
        return remote(
            source, lat.at[j, p, half], lat_side.at[j], lat_recv.at[j, p, half], place(other, t)
        )

    def lat_to_core(j, pp):
        spot = lat.at[j, pp, half]
        return remote(spot, spot, lat_core.at[j, pp], lat_recv.at[j, pp, half], place(p, mate))

    def lat_wait(j, pp, hh):
        spot = lat.at[j, pp, hh]
        remote(spot, spot, lat_up.at[0], lat_recv.at[j, pp, hh], place(p, mate)).wait_recv()

    stores = (gate, up, down)
    hidden_half = gate.shape[3]

    def piece(w, which):
        start = pl.multiple_of(which * hidden_half, 128)
        if w == 0:
            return gate_in.at[:, pl.ds(start, hidden_half)]
        if w == 1:
            return up_in.at[:, pl.ds(start, hidden_half)]
        return down_in.at[pl.ds(start, hidden_half), :]

    def w_to_side(w):
        return remote(
            piece(w, other),
            stores[w].at[q, p],
            w_side.at[w],
            w_recv.at[w, q, p],
            place(other, t),
        )

    def w_to_up(w, j, pp):
        spot = stores[w].at[j, pp]
        return remote(spot, spot, w_up.at[w, j, pp], w_recv.at[w, j, pp], place(p, t, q + 1))

    def w_to_down(w, j, pp):
        spot = stores[w].at[j, pp]
        return remote(spot, spot, w_down.at[w, j, pp], w_recv.at[w, j, pp], place(p, t, q - 1))

    def w_wait(w, j, pp):
        spot = stores[w].at[j, pp]
        remote(spot, spot, w_up.at[w, 0, 0], w_recv.at[w, j, pp], place(p, mate)).wait_recv()

    def w_own(w):
        return pltpu.make_async_copy(piece(w, p), stores[w].at[q, p], local_sem.at[1 + w])

    own_lat = pltpu.make_async_copy(latent_in, lat.at[q, p], local_sem.at[0])
    own_proj = pltpu.make_async_copy(proj_in, proj.at[t], local_sem.at[4])

    def proj_to(step):
        tt = lax.rem(t + step, teams)
        return remote(
            proj_in, proj.at[t], proj_send.at[step], proj_recv.at[step], place(p, tt)
        )

    own_lat.start()
    w_own(0).start()
    w_own(1).start()
    w_own(2).start()

    @pl.when(has_up)
    def _():
        lat_to_up(q, latent_in.at[half]).start()

    lat_to_side(q, latent_in.at[half]).start()
    for w in range(3):
        w_to_side(w).start()
    own_proj.start()
    for step in range(1, teams):
        proj_to(step).start()
    for w in range(3):
        w_own(w).wait()

        @pl.when(has_down)
        def _():
            w_to_down(w, q, p).start()

    top[...] = jnp.full_like(top, big_negative)
    total[...] = jnp.zeros_like(total)
    weighted[...] = jnp.zeros_like(weighted)

    def attend(j, pp, diagonal):
        block = lat[j, pp].reshape(block_rows, lat.shape[4])
        normed = block[:, :width]
        rotary = block[:, width:]
        keys = jnp.dot(normed, key_up[...], preferred_element_type=f32).astype(bf16)
        values = jnp.dot(normed, value_up[...], preferred_element_type=f32).astype(bf16)
        for h in range(head_count):
            span = slice(h * head_dim, (h + 1) * head_dim)
            both = jnp.concatenate([keys[:, span], rotary], axis=1)
            score = (
                lax.dot_general(
                    qcat[h], both, (((1,), (1,)), ((), ())), preferred_element_type=f32
                )
                * scale
            )
            if diagonal:
                across = lax.broadcasted_iota(jnp.int32, score.shape, 1)
                along = lax.broadcasted_iota(jnp.int32, score.shape, 0)
                score = jnp.where(across <= along, score, big_negative)
            old = top[h]
            new = jnp.maximum(old, jnp.max(score, axis=1, keepdims=True))
            powers = jnp.exp(score - new)
            shrink = jnp.exp(old - new)
            total[h] = total[h] * shrink + jnp.sum(powers, axis=1, keepdims=True)
            weighted[h] = weighted[h] * shrink + jnp.dot(
                powers.astype(bf16), values[:, span], preferred_element_type=f32
            )
            top[h] = new

    own_lat.wait()
    attend(q, p, True)

    for w in range(3):
        w_wait(w, q, other)

        @pl.when(has_down)
        def _():
            w_to_down(w, q, other).start()

    lat_wait(q, other, half)
    lat_to_core(q, other).start()

    def lat_step(s, carry):
        j = q - s

        @pl.when(j >= 0)
        def _():
            lat_wait(j, p, half)

            @pl.when(has_up)
            def _():
                lat_to_up(j, lat.at[j, p, half]).start()

            lat_to_side(j, lat.at[j, p, half]).start()
            lat_to_core(j, p).start()
            lat_wait(j, other, half)
            lat_to_core(j, other).start()

        return carry

    lax.fori_loop(1, chain, lat_step, 0)

    @pl.when(has_up)
    def _():
        for w in range(3):
            w_to_up(w, q, p).start()
            w_to_up(w, q, other).start()

    lat_wait(q, other, 1 - half)

    def whole_block(index, carry):
        j = q - (index + 1) // 2
        pp = jnp.where(index % 2 == 1, p, other)

        @pl.when(j >= 0)
        def _():
            @pl.when(index > 0)
            def _():
                lat_wait(j, pp, 1 - half)

            @pl.when((index > 0) | (p == 1))
            def _():
                attend(j, pp, False)

        return carry

    lax.fori_loop(0, 2 * chain - 1, whole_block, 0)

    part = block_rows // teams
    for h in range(head_count):
        span = slice(h * head_dim, (h + 1) * head_dim)
        done = (weighted[h] / total[h]).astype(bf16)
        heads_out[:, :, span] = done.reshape(teams, part, head_dim)

    def head_to(step):
        tt = lax.rem(t + step, teams)
        return remote(
            heads_out.at[tt], heads_in.at[t], head_send.at[step], head_recv.at[step], place(p, tt)
        )

    for step in range(1, teams):
        head_to(step).start()
    heads_in[t] = heads_out[t]

    def w_step(kinds, s):
        for w in kinds:
            for k in range(2):

                @pl.when(q - s >= 0)
                def _():
                    w_wait(w, q - s, k)

                    @pl.when(has_up)
                    def _():
                        w_to_up(w, q - s, k).start()

                @pl.when(q + s <= last)
                def _():
                    w_wait(w, q + s, k)

                    @pl.when(has_down)
                    def _():
                        w_to_down(w, q + s, k).start()

    def w_steps(kinds, first, end):
        def body(s, carry):
            w_step(kinds, s)
            return carry

        lax.fori_loop(first, end, body, 0)

    w_steps((0, 1), 1, 2)

    own_proj.wait()
    for step in range(1, teams):
        head_to(step).wait_recv()
        proj_to(step).wait_recv()

    def project(k, carry):
        wide[...] += jnp.dot(heads_in[k], proj[k], preferred_element_type=f32)
        return carry

    wide[...] = residual_weight * stream[...].astype(f32)
    lax.fori_loop(0, teams, project, 0)
    rows[mine] = layer_norm(wide[...], mix_gain[...]).astype(bf16)

    held = [(p, t)]
    slot = 0
    bits = []
    bit = 2
    while bit < teams:
        bits.append(bit)
        bit *= 2
    for stage in bits + [0, 1]:

        def flip(pp, tt):
            if stage == 0:
                return 1 - pp, tt
            return pp, jnp.where((tt // stage) % 2 == 0, tt + stage, tt - stage)

        partner = place(*flip(p, t))
        batch = []
        for pp, tt in held:
            spot = rows.at[pp * teams + tt]
            batch.append(
                remote(spot, spot, row_send.at[slot], row_recv.at[slot], partner)
            )
            slot += 1
        for copy in batch:
            copy.start()
        if stage == 0:
            w_steps((0, 1), 2, chain)
        for copy in batch:
            copy.wait()
        held = held + [flip(pp, tt) for pp, tt in held]

    def feed(k, carry):
        here = rows[pl.ds(2 * k, 2)].reshape(2 * part, rows.shape[2])
        gate_sum = jnp.dot(
            here, gate[...].reshape(-1, hidden_half), preferred_element_type=f32
        )
        up_sum = jnp.dot(here, up[...].reshape(-1, hidden_half), preferred_element_type=f32)
        value = gate_sum / (1.0 + jnp.exp(-gate_sum)) * up_sum
        hidden[pl.ds(2 * k, 2)] = value.astype(bf16).reshape(2, part, hidden_half)
        return carry

    lax.fori_loop(0, group // 2, feed, 0)

    def term_to(j, step):
        index = lax.rem(mine + step, group)
        return remote(
            terms.at[j, index],
            arrived.at[j, mine],
            term_send.at[j, step],
            term_recv.at[j, step],
            place(index // teams, index % teams),
        )

    def lower(j):
        weights = jnp.concatenate([down[j, 0], down[j, 1]], axis=1)
        product = jnp.dot(
            hidden[...].reshape(group * part, hidden_half), weights, preferred_element_type=f32
        )
        terms[j] = product.astype(bf16).reshape(group, part, product.shape[1])
        for step in range(1, group):
            term_to(j, step).start()

    lower(q)

    def lower_step(s, carry):
        w_step((2,), s)

        def one(side, inner):
            j = jnp.where(side == 0, q - s, q + s)

            @pl.when((j >= 0) & (j <= last))
            def _():
                lower(j)

            return inner

        lax.fori_loop(0, 2, one, 0)
        return carry

    lax.fori_loop(1, chain, lower_step, 0)

    def collect(j, carry):
        for step in range(1, group):
            term_to(j, step).wait()
        return carry

    lax.fori_loop(0, chain, collect, 0)
    span_width = terms.shape[3]
    for j in range(chain):
        arrived[j, mine] = terms[j, mine]
        lowered = arrived[j, 0].astype(f32)
        for k in range(1, group):
            lowered = lowered + arrived[j, k].astype(f32)
        span = slice(j * span_width, (j + 1) * span_width)
        wide[:, span] = residual_weight * rows[mine, :, span].astype(f32) + 0.5 * lowered
    result[...] = layer_norm(wide[...], mlp_gain[...]).astype(bf16)

    for w in range(3):
        w_to_side(w).wait_send()
    for step in range(1, teams):
        proj_to(step).wait_send()
        head_to(step).wait_send()

    def drain(j, carry):
        @pl.when(has_up & (j <= q))
        def _():
            lat_to_up(j, lat.at[j, p, half]).wait_send()
            for w in range(3):
                for k in range(2):
                    w_to_up(w, j, k).wait_send()

        @pl.when(has_down & (j >= q))
        def _():
            for w in range(3):
                for k in range(2):
                    w_to_down(w, j, k).wait_send()

        @pl.when(j <= q)
        def _():
            lat_to_side(j, lat.at[j, p, half]).wait_send()
            lat_to_core(j, other).wait_send()

        @pl.when(j < q)
        def _():
            lat_to_core(j, p).wait_send()

        return carry

    lax.fori_loop(0, chain, drain, 0)


def per_device(
    chain,
    teams,
    queries_nope,
    queries_rope,
    latent,
    rope_key,
    latent_gain,
    key_up,
    value_up,
    out_proj,
    stream,
    mix_gain,
    w_gate,
    w_up,
    w_down,
    mlp_gain,
):
    row_count, head_count, head_dim = queries_nope.shape
    rope_dim = queries_rope.shape[2]
    first_row = lax.axis_index("sp") * row_count
    query_turned = rotate(queries_rope.astype(jnp.float32), first_row).astype(jnp.bfloat16)
    key_turned = rotate(rope_key.astype(jnp.float32), first_row).astype(jnp.bfloat16)
    normed = latent_norm(latent, latent_gain)
    scale = (head_dim + rope_dim) ** (-0.5)
    spare = -rope_dim % 128
    qcat = jnp.concatenate(
        [queries_nope, query_turned, jnp.zeros((row_count, head_count, spare), bf16)], axis=2
    ).transpose(1, 0, 2)
    latent_in = jnp.concatenate(
        [normed, key_turned, jnp.zeros((row_count, spare), bf16)], axis=1
    ).reshape(2, row_count // 2, -1)
    width = latent_in.shape[2]
    model, hidden_here = w_gate.shape[0] * 2 * chain, w_gate.shape[1]
    group = 2 * teams
    part = row_count // teams
    half_hidden = hidden_here // 2
    deep = w_gate.shape[0]
    slim = w_down.shape[1]
    stages = group - 1
    dma = pltpu.SemaphoreType.DMA
    vmem = pl.BlockSpec(memory_space=pltpu.VMEM)
    hbm = pl.BlockSpec(memory_space=pltpu.HBM)
    return pl.pallas_call(
        functools.partial(layer_kernel, chain, teams, scale),
        out_shape=jax.ShapeDtypeStruct((part, model), bf16),
        in_specs=[vmem, hbm, vmem, vmem, hbm, vmem, vmem, hbm, hbm, hbm, vmem],
        out_specs=vmem,
        scratch_shapes=[
            pltpu.VMEM((chain, 2, 2, row_count // 2, width), bf16),
            pltpu.VMEM((chain, 2, deep, half_hidden), bf16),
            pltpu.VMEM((chain, 2, deep, half_hidden), bf16),
            pltpu.VMEM((chain, 2, half_hidden, slim), bf16),
            pltpu.VMEM((teams,) + out_proj.shape, bf16),
            pltpu.VMEM((teams, part, head_count * head_dim), bf16),
            pltpu.VMEM((teams, part, head_count * head_dim), bf16),
            pltpu.VMEM((group, part, model), bf16),
            pltpu.VMEM((group, part, half_hidden), bf16),
            pltpu.VMEM((chain, group, part, 2 * slim), bf16),
            pltpu.VMEM((chain, group, part, 2 * slim), bf16),
            pltpu.VMEM((part, model), f32),
            pltpu.VMEM((head_count, row_count, 1), f32),
            pltpu.VMEM((head_count, row_count, 1), f32),
            pltpu.VMEM((head_count, row_count, head_dim), f32),
            dma((5,)),
            dma((chain, 2, 2)),
            dma((chain,)),
            dma((chain,)),
            dma((chain, 2)),
            dma((3, chain, 2)),
            dma((3,)),
            dma((3, chain, 2)),
            dma((3, chain, 2)),
            dma((teams,)),
            dma((teams,)),
            dma((teams,)),
            dma((teams,)),
            dma((stages,)),
            dma((stages,)),
            dma((chain, group)),
            dma((chain, group)),
        ],
        compiler_params=pltpu.CompilerParams(
            collective_id=0, has_side_effects=True, vmem_limit_bytes=60 * 1024 * 1024
        ),
    )(
        qcat,
        latent_in,
        key_up,
        value_up,
        out_proj,
        stream,
        mix_gain.reshape(1, -1),
        w_gate,
        w_up,
        w_down,
        mlp_gain.reshape(1, -1),
    )


def solution(mesh):
    return jax.shard_map(
        functools.partial(per_device, mesh.shape["sp"] // 2, mesh.shape["tp"]),
        mesh=mesh,
        in_specs=(
            P("sp", "tp", None),
            P("sp", "tp", None),
            P("sp", None),
            P("sp", None),
            P(),
            P(None, "tp"),
            P(None, "tp"),
            P("tp", None),
            P(("sp", "tp"), None),
            P(),
            P("sp", "tp"),
            P("sp", "tp"),
            P("tp", "sp"),
            P(),
        ),
        out_specs=P(("sp", "tp"), None),
        check_vma=False,
    )
```

```python
import functools

import jax
import jax.numpy as jnp
from jax import lax
from jax.experimental import pallas as pl
from jax.experimental.pallas import tpu as pltpu
from jax.sharding import PartitionSpec as P

theta_base = 10000.0
residual_weight = 8.0**0.25
norm_floor = 1.0
big_negative = -1e30


def rotate(vector, first_row):
    half = vector.shape[-1] // 2
    rates = theta_base ** (-2.0 * jnp.arange(half, dtype=jnp.float32) / vector.shape[-1])
    places = (first_row + jnp.arange(vector.shape[0], dtype=jnp.int32)).astype(jnp.float32)
    angle = places[:, None] * rates[None, :]
    angle = angle.reshape((vector.shape[0],) + (1,) * (vector.ndim - 2) + (half,))
    cosine = jnp.cos(angle)
    sine = jnp.sin(angle)
    left = vector[..., :half]
    right = vector[..., half:]
    return jnp.concatenate([left * cosine - right * sine, left * sine + right * cosine], axis=-1)


def latent_norm(latent, latent_gain):
    wide = latent.astype(jnp.float32)
    factor = lax.rsqrt(jnp.mean(wide * wide, axis=-1, keepdims=True) + norm_floor)
    return (wide * factor * latent_gain).astype(jnp.bfloat16)


def layer_norm(values, gain):
    centre = jnp.mean(values, axis=-1, keepdims=True)
    centred = values - centre
    spread = jnp.mean(centred * centred, axis=-1, keepdims=True)
    return centred * lax.rsqrt(spread + norm_floor) * gain


mesh_id = pl.DeviceIdType.MESH
bf16 = jnp.bfloat16
f32 = jnp.float32


def layer_kernel(
    chain,
    teams,
    scale,
    qcat,
    latent_in,
    key_up,
    value_up,
    proj_in,
    stream,
    mix_gain,
    gate_in,
    up_in,
    down_in,
    mlp_gain,
    result,
    lat,
    gate,
    up,
    down,
    proj,
    heads_out,
    heads_in,
    rows,
    hidden,
    terms_out,
    mate_in,
    terms,
    arrived,
    wide,
    top,
    total,
    weighted,
    local_sem,
    lat_recv,
    lat_up,
    lat_side,
    lat_core,
    w_recv,
    w_side,
    w_up,
    w_down,
    proj_recv,
    proj_send,
    head_recv,
    head_send,
    row_recv,
    row_send,
    mate_recv,
    mate_send,
    term_recv,
    term_send,
):
    sp = lax.axis_index("sp")
    t = lax.axis_index("tp")
    q = sp // 2
    p = sp % 2
    other = 1 - p
    half = t % 2
    mate = t + 1 - 2 * half
    group = 2 * teams
    mine = half * teams + p * (teams // 2) + t // 2
    own_class = half * teams
    last = chain - 1
    head_count = qcat.shape[0]
    head_dim = value_up.shape[1] // head_count
    block_rows = qcat.shape[1]
    width = value_up.shape[0]
    has_up = q < last
    has_down = q > 0

    def place(pp, tt, qq=None):
        return ((q if qq is None else qq) * 2 + pp, tt)

    def remote(source, target, send, recv, device):
        return pltpu.make_async_remote_copy(
            src_ref=source,
            dst_ref=target,
            send_sem=send,
            recv_sem=recv,
            device_id=device,
            device_id_type=mesh_id,
        )

    barrier = pltpu.get_barrier_semaphore()
    place_here = p * teams + t
    for step in range(1, group):
        index = lax.rem(place_here + step, group)
        pl.semaphore_signal(
            barrier, inc=1, device_id=place(index // teams, index % teams), device_id_type=mesh_id
        )

    @pl.when(has_up)
    def _():
        pl.semaphore_signal(barrier, inc=1, device_id=place(p, t, q + 1), device_id_type=mesh_id)

    @pl.when(has_down)
    def _():
        pl.semaphore_signal(barrier, inc=1, device_id=place(p, t, q - 1), device_id_type=mesh_id)

    peers = group - 1 + jnp.where(has_up, 1, 0) + jnp.where(has_down, 1, 0)
    pl.semaphore_wait(barrier, peers)

    def lat_to_up(j, source):
        return remote(
            source, lat.at[j, p, half], lat_up.at[j], lat_recv.at[j, p, half], place(p, t, q + 1)
        )

    def lat_to_side(j, source):
        return remote(
            source, lat.at[j, p, half], lat_side.at[j], lat_recv.at[j, p, half], place(other, t)
        )

    def lat_to_core(j, pp):
        spot = lat.at[j, pp, half]
        return remote(spot, spot, lat_core.at[j, pp], lat_recv.at[j, pp, half], place(p, mate))

    def lat_wait(j, pp, hh):
        spot = lat.at[j, pp, hh]
        remote(spot, spot, lat_up.at[0], lat_recv.at[j, pp, hh], place(p, mate)).wait_recv()

    stores = (gate, up, down)
    hidden_half = gate.shape[3]

    def piece(w, which):
        start = pl.multiple_of(which * hidden_half, 128)
        if w == 0:
            return gate_in.at[:, pl.ds(start, hidden_half)]
        if w == 1:
            return up_in.at[:, pl.ds(start, hidden_half)]
        return down_in.at[pl.ds(start, hidden_half), :]

    def w_to_side(w):
        return remote(
            piece(w, other),
            stores[w].at[q, p],
            w_side.at[w],
            w_recv.at[w, q, p],
            place(other, t),
        )

    def w_to_up(w, j, pp):
        spot = stores[w].at[j, pp]
        return remote(spot, spot, w_up.at[w, j, pp], w_recv.at[w, j, pp], place(p, t, q + 1))

    def w_to_down(w, j, pp):
        spot = stores[w].at[j, pp]
        return remote(spot, spot, w_down.at[w, j, pp], w_recv.at[w, j, pp], place(p, t, q - 1))

    def w_wait(w, j, pp):
        spot = stores[w].at[j, pp]
        remote(spot, spot, w_up.at[w, 0, 0], w_recv.at[w, j, pp], place(p, mate)).wait_recv()

    def w_own(w):
        return pltpu.make_async_copy(piece(w, p), stores[w].at[q, p], local_sem.at[1 + w])

    own_lat = pltpu.make_async_copy(latent_in, lat.at[q, p], local_sem.at[0])
    own_proj = pltpu.make_async_copy(proj_in, proj.at[t], local_sem.at[4])

    def proj_to(step):
        tt = lax.rem(t + step, teams)
        return remote(proj_in, proj.at[t], proj_send.at[step], proj_recv.at[step], place(p, tt))

    def proj_mate():
        return remote(proj_in, proj.at[t], proj_send.at[1], proj_recv.at[1], place(p, mate))

    def proj_pass(step):
        spot = proj.at[lax.rem(t - step + teams, teams)]
        return remote(spot, spot, proj_send.at[step + 1], proj_recv.at[step + 1], place(p, mate))

    own_lat.start()
    w_own(0).start()
    w_own(1).start()
    w_own(2).start()

    @pl.when(has_up)
    def _():
        lat_to_up(q, latent_in.at[half]).start()

    lat_to_side(q, latent_in.at[half]).start()
    for w in range(3):
        w_to_side(w).start()
    own_proj.start()
    for step in range(2, teams, 2):
        proj_to(step).start()
    proj_mate().start()
    for w in range(3):
        w_own(w).wait()

        @pl.when(has_down)
        def _():
            w_to_down(w, q, p).start()

    top[...] = jnp.full_like(top, big_negative)
    total[...] = jnp.zeros_like(total)
    weighted[...] = jnp.zeros_like(weighted)

    def attend(j, pp, diagonal):
        block = lat[j, pp].reshape(block_rows, lat.shape[4])
        normed = block[:, :width]
        rotary = block[:, width:]
        keys = jnp.dot(normed, key_up[...], preferred_element_type=f32).astype(bf16)
        values = jnp.dot(normed, value_up[...], preferred_element_type=f32).astype(bf16)
        for h in range(head_count):
            span = slice(h * head_dim, (h + 1) * head_dim)
            both = jnp.concatenate([keys[:, span], rotary], axis=1)
            score = (
                lax.dot_general(
                    qcat[h], both, (((1,), (1,)), ((), ())), preferred_element_type=f32
                )
                * scale
            )
            if diagonal:
                across = lax.broadcasted_iota(jnp.int32, score.shape, 1)
                along = lax.broadcasted_iota(jnp.int32, score.shape, 0)
                score = jnp.where(across <= along, score, big_negative)
            old = top[h]
            new = jnp.maximum(old, jnp.max(score, axis=1, keepdims=True))
            powers = jnp.exp(score - new)
            shrink = jnp.exp(old - new)
            total[h] = total[h] * shrink + jnp.sum(powers, axis=1, keepdims=True)
            weighted[h] = weighted[h] * shrink + jnp.dot(
                powers.astype(bf16), values[:, span], preferred_element_type=f32
            )
            top[h] = new

    own_lat.wait()
    attend(q, p, True)

    for w in range(3):
        w_wait(w, q, other)

        @pl.when(has_down)
        def _():
            w_to_down(w, q, other).start()

    lat_wait(q, other, half)
    lat_to_core(q, other).start()

    def lat_step(s, carry):
        j = q - s

        @pl.when(j >= 0)
        def _():
            lat_wait(j, p, half)

            @pl.when(has_up)
            def _():
                lat_to_up(j, lat.at[j, p, half]).start()

            lat_to_side(j, lat.at[j, p, half]).start()
            lat_to_core(j, p).start()
            lat_wait(j, other, half)
            lat_to_core(j, other).start()

        return carry

    lax.fori_loop(1, chain, lat_step, 0)

    @pl.when(has_up)
    def _():
        for w in range(2):
            w_to_up(w, q, p).start()
            w_to_up(w, q, other).start()

    lat_wait(q, other, 1 - half)

    def whole_block(index, carry):
        j = q - (index + 1) // 2
        pp = jnp.where(index % 2 == 1, p, other)

        @pl.when(j >= 0)
        def _():
            @pl.when(index > 0)
            def _():
                lat_wait(j, pp, 1 - half)

            @pl.when((index > 0) | (p == 1))
            def _():
                attend(j, pp, False)

        return carry

    lax.fori_loop(0, 2 * chain - 1, whole_block, 0)

    part = block_rows // teams
    for h in range(head_count):
        span = slice(h * head_dim, (h + 1) * head_dim)
        done = (weighted[h] / total[h]).astype(bf16)
        heads_out[:, :, span] = done.reshape(teams, part, head_dim)

    def head_to(step):
        tt = lax.rem(t + step, teams)
        return remote(
            heads_out.at[tt], heads_in.at[t], head_send.at[step], head_recv.at[step], place(p, tt)
        )

    for step in range(1, teams):
        head_to(step).start()
    heads_in[t] = heads_out[t]

    def w_step(kinds, s):
        for w in kinds:
            for k in range(2):

                @pl.when(q - s >= 0)
                def _():
                    w_wait(w, q - s, k)

                    @pl.when(has_up)
                    def _():
                        w_to_up(w, q - s, k).start()

                @pl.when(q + s <= last)
                def _():
                    w_wait(w, q + s, k)

                    @pl.when(has_down)
                    def _():
                        w_to_down(w, q + s, k).start()

    def w_steps(kinds, first, end):
        def body(s, carry):
            w_step(kinds, s)
            return carry

        lax.fori_loop(first, end, body, 0)

    for step in range(2, teams, 2):
        proj_to(step).wait_recv()
        proj_pass(step).start()
    w_steps((0, 1), 1, 2)

    @pl.when(has_up)
    def _():
        w_to_up(2, q, p).start()
        w_to_up(2, q, other).start()

    own_proj.wait()
    proj_mate().wait_recv()
    for step in range(1, teams):
        head_to(step).wait_recv()
    for step in range(2, teams, 2):
        proj_pass(step).wait_recv()

    def project(k, carry):
        wide[...] += jnp.dot(heads_in[k], proj[k], preferred_element_type=f32)
        return carry

    wide[...] = residual_weight * stream[...].astype(f32)
    lax.fori_loop(0, teams, project, 0)
    rows[mine] = layer_norm(wide[...], mix_gain[...]).astype(bf16)

    stages = []
    bit = 2
    while bit < teams:
        stages.append(bit)
        bit *= 2
    stages += [0, 1]

    def flip(stage, pp, tt):
        if stage == 0:
            return 1 - pp, tt
        return pp, jnp.where((tt // stage) % 2 == 0, tt + stage, tt - stage)

    held = [(p, t)]
    for stage in stages:
        held = held + [flip(stage, pp, tt) for pp, tt in held]

    def row_copy(i, u):
        pp, tt = held[u]
        spot = rows.at[(tt % 2) * teams + pp * (teams // 2) + tt // 2]
        slot = 2**i - 1 + u
        partner = place(*flip(stages[i], p, t))
        return remote(spot, spot, row_send.at[slot], row_recv.at[slot], partner)

    for i in range(len(stages)):
        row_copy(i, 0).start()
    for i in range(len(stages)):
        for u in range(2**i):
            row_copy(i, u).wait_recv()
            for later in range(i + 1, len(stages)):
                row_copy(later, 2**i + u).start()
    w_steps((0, 1), 2, chain)

    def feed(k, carry):
        here = rows[pl.ds(2 * k, 2)].reshape(2 * part, rows.shape[2])
        gate_sum = jnp.dot(
            here, gate[...].reshape(-1, hidden_half), preferred_element_type=f32
        )
        up_sum = jnp.dot(here, up[...].reshape(-1, hidden_half), preferred_element_type=f32)
        value = gate_sum / (1.0 + jnp.exp(-gate_sum)) * up_sum
        hidden[pl.ds(2 * k, 2)] = value.astype(bf16).reshape(2, part, hidden_half)
        return carry

    lax.fori_loop(0, group // 2, feed, 0)

    my_turn = p * (teams // 2) + t // 2

    def term_mate(j):
        return remote(
            terms_out.at[j], mate_in.at[j], mate_send.at[j], mate_recv.at[j], place(p, mate)
        )

    def term_to(j, step):
        index = lax.rem(my_turn + step, teams)
        pp = index // (teams // 2)
        tt = 2 * (index % (teams // 2)) + half
        return remote(
            terms.at[j, index],
            arrived.at[j, my_turn],
            term_send.at[j, step],
            term_recv.at[j, step],
            place(pp, tt),
        )

    def lower(j):
        weights = jnp.concatenate([down[j, 0], down[j, 1]], axis=1)

        def product(first):
            here = hidden[pl.ds(first, teams)].reshape(teams * part, hidden_half)
            return jnp.dot(here, weights, preferred_element_type=f32)

        there = product(teams - own_class)
        terms_out[j] = there.astype(bf16).reshape(teams, part, there.shape[1])
        term_mate(j).start()
        kept = product(own_class)
        term_mate(j).wait_recv()
        kept = kept.reshape(teams, part, kept.shape[1]) + mate_in[j].astype(f32)
        terms[j] = kept.astype(bf16)
        for step in range(1, teams):
            term_to(j, step).start()

    lower(q)

    def lower_step(s, carry):
        w_step((2,), s)

        def one(side, inner):
            j = jnp.where(side == 0, q - s, q + s)

            @pl.when((j >= 0) & (j <= last))
            def _():
                lower(j)

            return inner

        lax.fori_loop(0, 2, one, 0)
        return carry

    lax.fori_loop(1, chain, lower_step, 0)

    def collect(j, carry):
        for step in range(1, teams):
            term_to(j, step).wait()
        return carry

    lax.fori_loop(0, chain, collect, 0)
    span_width = terms.shape[3]
    for j in range(chain):
        arrived[j, my_turn] = terms[j, my_turn]
        lowered = arrived[j, 0].astype(f32)
        for k in range(1, teams):
            lowered = lowered + arrived[j, k].astype(f32)
        span = slice(j * span_width, (j + 1) * span_width)
        wide[:, span] = residual_weight * rows[mine, :, span].astype(f32) + 0.5 * lowered
    result[...] = layer_norm(wide[...], mlp_gain[...]).astype(bf16)

    for w in range(3):
        w_to_side(w).wait_send()
    proj_mate().wait_send()
    for step in range(2, teams, 2):
        proj_to(step).wait_send()
        proj_pass(step).wait_send()
    for step in range(1, teams):
        head_to(step).wait_send()
    for i in range(len(stages)):
        for u in range(2**i):
            row_copy(i, u).wait_send()

    def drain(j, carry):
        term_mate(j).wait_send()

        @pl.when(has_up & (j <= q))
        def _():
            lat_to_up(j, lat.at[j, p, half]).wait_send()
            for w in range(3):
                for k in range(2):
                    w_to_up(w, j, k).wait_send()

        @pl.when(has_down & (j >= q))
        def _():
            for w in range(3):
                for k in range(2):
                    w_to_down(w, j, k).wait_send()

        @pl.when(j <= q)
        def _():
            lat_to_side(j, lat.at[j, p, half]).wait_send()
            lat_to_core(j, other).wait_send()

        @pl.when(j < q)
        def _():
            lat_to_core(j, p).wait_send()

        return carry

    lax.fori_loop(0, chain, drain, 0)


def per_device(
    chain,
    teams,
    queries_nope,
    queries_rope,
    latent,
    rope_key,
    latent_gain,
    key_up,
    value_up,
    out_proj,
    stream,
    mix_gain,
    w_gate,
    w_up,
    w_down,
    mlp_gain,
):
    row_count, head_count, head_dim = queries_nope.shape
    rope_dim = queries_rope.shape[2]
    first_row = lax.axis_index("sp") * row_count
    query_turned = rotate(queries_rope.astype(jnp.float32), first_row).astype(jnp.bfloat16)
    key_turned = rotate(rope_key.astype(jnp.float32), first_row).astype(jnp.bfloat16)
    normed = latent_norm(latent, latent_gain)
    scale = (head_dim + rope_dim) ** (-0.5)
    spare = -rope_dim % 128
    qcat = jnp.concatenate(
        [queries_nope, query_turned, jnp.zeros((row_count, head_count, spare), bf16)], axis=2
    ).transpose(1, 0, 2)
    latent_in = jnp.concatenate(
        [normed, key_turned, jnp.zeros((row_count, spare), bf16)], axis=1
    ).reshape(2, row_count // 2, -1)
    width = latent_in.shape[2]
    model, hidden_here = w_gate.shape[0] * 2 * chain, w_gate.shape[1]
    group = 2 * teams
    part = row_count // teams
    half_hidden = hidden_here // 2
    deep = w_gate.shape[0]
    slim = w_down.shape[1]
    stages = group - 1
    dma = pltpu.SemaphoreType.DMA
    vmem = pl.BlockSpec(memory_space=pltpu.VMEM)
    hbm = pl.BlockSpec(memory_space=pltpu.HBM)
    return pl.pallas_call(
        functools.partial(layer_kernel, chain, teams, scale),
        out_shape=jax.ShapeDtypeStruct((part, model), bf16),
        in_specs=[vmem, hbm, vmem, vmem, hbm, vmem, vmem, hbm, hbm, hbm, vmem],
        out_specs=vmem,
        scratch_shapes=[
            pltpu.VMEM((chain, 2, 2, row_count // 2, width), bf16),
            pltpu.VMEM((chain, 2, deep, half_hidden), bf16),
            pltpu.VMEM((chain, 2, deep, half_hidden), bf16),
            pltpu.VMEM((chain, 2, half_hidden, slim), bf16),
            pltpu.VMEM((teams,) + out_proj.shape, bf16),
            pltpu.VMEM((teams, part, head_count * head_dim), bf16),
            pltpu.VMEM((teams, part, head_count * head_dim), bf16),
            pltpu.VMEM((group, part, model), bf16),
            pltpu.VMEM((group, part, half_hidden), bf16),
            pltpu.VMEM((chain, teams, part, 2 * slim), bf16),
            pltpu.VMEM((chain, teams, part, 2 * slim), bf16),
            pltpu.VMEM((chain, teams, part, 2 * slim), bf16),
            pltpu.VMEM((chain, teams, part, 2 * slim), bf16),
            pltpu.VMEM((part, model), f32),
            pltpu.VMEM((head_count, row_count, 1), f32),
            pltpu.VMEM((head_count, row_count, 1), f32),
            pltpu.VMEM((head_count, row_count, head_dim), f32),
            dma((5,)),
            dma((chain, 2, 2)),
            dma((chain,)),
            dma((chain,)),
            dma((chain, 2)),
            dma((3, chain, 2)),
            dma((3,)),
            dma((3, chain, 2)),
            dma((3, chain, 2)),
            dma((teams,)),
            dma((teams,)),
            dma((teams,)),
            dma((teams,)),
            dma((stages,)),
            dma((stages,)),
            dma((chain,)),
            dma((chain,)),
            dma((chain, teams)),
            dma((chain, teams)),
        ],
        compiler_params=pltpu.CompilerParams(
            collective_id=0, has_side_effects=True, vmem_limit_bytes=60 * 1024 * 1024
        ),
    )(
        qcat,
        latent_in,
        key_up,
        value_up,
        out_proj,
        stream,
        mix_gain.reshape(1, -1),
        w_gate,
        w_up,
        w_down,
        mlp_gain.reshape(1, -1),
    )


def solution(mesh):
    return jax.shard_map(
        functools.partial(per_device, mesh.shape["sp"] // 2, mesh.shape["tp"]),
        mesh=mesh,
        in_specs=(
            P("sp", "tp", None),
            P("sp", "tp", None),
            P("sp", None),
            P("sp", None),
            P(),
            P(None, "tp"),
            P(None, "tp"),
            P("tp", None),
            P(("sp", "tp"), None),
            P(),
            P("sp", "tp"),
            P("sp", "tp"),
            P("tp", "sp"),
            P(),
        ),
        out_specs=P(("sp", "tp"), None),
        check_vma=False,
    )
```
